256 devices in a mesh: fs: 32 (over z, x), tp: 8 (over y, core).
Axes of the slice: x: 4, y: 4, z: 8, core: 2. Of those that a mesh axis runs over, the one named last changes fastest.
Arguments:
- normed_input: bfloat16 [65536, 2048], P('fs'), may hold values from -6 to 6
- gate_cotangent: bfloat16 [65536, 2048], P('fs', 'tp'), may hold values from -0.0625 to 0.0625
- first_value_cot: bfloat16 [65536, 1024], P('fs', 'tp'), may hold values from -0.0625 to 0.0625
- second_value_cot: bfloat16 [65536, 1024], P('fs', 'tp'), may hold values from -0.0625 to 0.0625
- head_lambda: float32 [8], P('tp'), may hold values from 0.3 to 0.8
- projection: bfloat16 [2048, 256], replicated, may hold values from -1 to 1, as said below
- gate_weight: float32 [2048, 2048], P('fs', 'tp'), may hold values from -0.125 to 0.125
- gate_first: float32 [256, 2048], P('fs', 'tp'), may hold values from -1.5 to 1.5
- gate_second: float32 [256, 2048], P('fs', 'tp'), may hold values from 0.01 to 1
- value_weight: float32 [2048, 1024], P('fs', 'tp'), may hold values from -0.125 to 0.125
- value_first: float32 [256, 1024], P('fs', 'tp'), may hold values from -1.5 to 1.5
- value_second: float32 [256, 1024], P('fs', 'tp'), may hold values from 0.01 to 1
Outputs:
- new_gate_weight: float32 [2048, 2048], P('fs', 'tp')
- gate_step: float32 [2048, 2048], P('fs', 'tp')
- gate_copy: bfloat16 [2048, 2048], P(None, 'tp')
- new_gate_first: float32 [256, 2048], P('fs', 'tp')
- new_gate_second: float32 [256, 2048], P('fs', 'tp')
- new_value_weight: float32 [2048, 1024], P('fs', 'tp')
- value_step: float32 [2048, 1024], P('fs', 'tp')
- value_copy: bfloat16 [2048, 1024], P(None, 'tp')
- new_value_first: float32 [256, 1024], P('fs', 'tp')
- new_value_second: float32 [256, 1024], P('fs', 'tp')
The draws below stay inside these ranges and needn't reach their ends.
Inputs may be any that keep to these rules, and one draw needn't show every extreme that they name: `projection`: a low-rank factor whose rows differ in scale.
All inputs are finite; a program needn't handle non-finite values.
Results may differ from the reference program's by a relative error of at most 0.0054.
Values may be sent and summed in bfloat16 or wider, within the bound.
A program may use at most 64 MiB of HBM per device.

```python
import math
import jax
import jax.numpy as jnp
from jax import lax

D = 2048
HEADS = 8
VDIM = 128
RANK = 256
TOKENS = 65536


def draw_projection(key, part):
    noise_key = jax.random.fold_in(key, 11)
    rough_key = jax.random.fold_in(key, 12)
    phase_key = jax.random.fold_in(key, 13)
    row_place = jnp.arange(D, dtype=jnp.float32)[:, None] / D
    phase = jax.random.uniform(phase_key, (), jnp.float32, 0.0, 6.2832)
    slow = jnp.exp(1.2 * jnp.sin(12.566 * row_place + phase))
    rough = jnp.exp(jax.random.uniform(rough_key, (D, 1), jnp.float32, -0.5, 0.5))
    base = jax.random.normal(noise_key, (D, RANK), jnp.float32)
    value = base * slow * rough * D ** (-0.5)
    return jnp.clip(value, -1.0, 1.0).astype(jnp.bfloat16)


def raised(entries, key, source, target, shards_of, factor):
    owner, partner = [(jnp.arange(entries.shape[axis_at]) // (entries.shape[axis_at] // shards_of)).reshape([-1 if axis == axis_at else 1 for axis in range(entries.ndim)]) for axis_at in (source, target)]
    chosen = jax.random.permutation(key, shards_of)[partner]
    strong = (owner == chosen) | (owner == (partner + shards_of // 2) % shards_of)
    return jnp.where(strong, factor * entries, entries)


def steps_of(key, dims, split, smallest, largest):
    loudness = 1.0
    for axis_at, blocks in split:
        heights = jax.random.uniform(jax.random.fold_in(jax.random.fold_in(key, 6), axis_at), (blocks,), jnp.float32, smallest / len(split), largest / len(split))
        loudness = loudness * jnp.repeat(jnp.exp(heights), dims[axis_at] // blocks).reshape((-1,) + (1,) * (len(dims) - 1 - axis_at))
    return loudness


def noise(own_key, dims, spread, bound, cuts=(), held_as=jnp.bfloat16):
    array = spread * jax.random.normal(own_key, dims, jnp.float32)
    if cuts:
        array = array * steps_of(own_key, dims, cuts, -0.22, 0.18)
    return jnp.clip(array, -bound, bound).astype(held_as)


def gaussian_with(key, extent, deviation, limit, shards, heavy, kind=jnp.bfloat16):
    array = deviation * jax.random.normal(key, extent, jnp.float32)
    if shards:
        array = array * steps_of(key, extent, shards, -0.22, 0.18)
    return jnp.clip(raised(array, jax.random.fold_in(key, 3), *heavy), -limit, limit).astype(kind)


def setup_inputs(seed: int = 0) -> dict:
    splits = jax.random.split(jax.random.key(seed), 13)
    return {
        "normed_input": gaussian_with(splits[0], (TOKENS, D), 1.0, 6.0, ((0, 32),), (0, 1, 32, 2.75)),
        "gate_cotangent": noise(splits[1], (TOKENS, D), (TOKENS ** -0.5), 0.0625, ((0, 32), (1, 8))),
        "first_value_cot": noise(splits[2], (TOKENS, HEADS * VDIM), (TOKENS ** -0.5), 0.0625, ((0, 32), (1, 8))),
        "second_value_cot": noise(splits[3], (TOKENS, HEADS * VDIM), (TOKENS ** -0.5), 0.0625, ((0, 32), (1, 8))),
        "head_lambda": jnp.clip(0.3 + 0.5 * jax.random.uniform(splits[4], (HEADS,), jnp.float32) ** steps_of(splits[4], (HEADS,), ((0, 8),), -0.2, 0.2), 0.3, 0.8),
        "projection": draw_projection(jax.random.fold_in(splits[12], 71), 0),
        "gate_weight": noise(splits[6], (D, D), D ** -0.5, 0.125, ((0, 32), (1, 8)), jnp.float32),
        "gate_first": noise(splits[7], (RANK, D), 0.1, 1.5, ((0, 32), (1, 8)), jnp.float32),
        "gate_second": jnp.clip(jnp.exp(math.log(1.0) - 4.6051702 * jax.random.uniform(splits[8], (RANK, D), jnp.float32) ** steps_of(splits[8], (RANK, D), ((0, 32), (1, 8)), -0.2, 0.2)), 0.01, 1.0),
        "value_weight": noise(splits[9], (D, HEADS * VDIM), D ** -0.5, 0.125, ((0, 32), (1, 8)), jnp.float32),
        "value_first": noise(splits[10], (RANK, HEADS * VDIM), 0.1, 1.5, ((0, 32), (1, 8)), jnp.float32),
        "value_second": jnp.clip(jnp.exp(math.log(1.0) - 4.6051702 * jax.random.uniform(splits[11], (RANK, HEADS * VDIM), jnp.float32) ** steps_of(splits[11], (RANK, HEADS * VDIM), ((0, 32), (1, 8)), -0.2, 0.2)), 0.01, 1.0),
    }


moment_decay = 0.9
square_decay = 0.95
adam_floor = 1e-08
learn_rate = 0.02
rms_floor = 0.1

def across_tokens(left, right):
    return lax.dot_general(left, right, (((0,), (0,)), ((), ())), preferred_element_type=jnp.float32)

def optimizer_step(weight, first, second, gradient, projection):
    factor = projection.astype(jnp.float32)
    low = lax.dot_general(factor, gradient, (((0,), (0,)), ((), ())), precision=lax.Precision.HIGHEST)
    new_first = moment_decay * first + (1.0 - moment_decay) * low
    new_second = square_decay * second + (1.0 - square_decay) * low * low
    direction = new_first / (jnp.sqrt(new_second) + adam_floor)
    update = jnp.dot(factor, direction, precision=lax.Precision.HIGHEST)
    step = update / (jnp.sqrt(jnp.mean(update * update)) + rms_floor)
    new_weight = weight - learn_rate * step
    return (new_weight, step, new_weight.astype(jnp.bfloat16), new_first, new_second)

def reference(normed_input, gate_cotangent, first_value_cot, second_value_cot, head_lambda, projection, gate_weight, gate_first, gate_second, value_weight, value_first, value_second):
    column_lambda = jnp.repeat(head_lambda, VDIM)
    value_cot = (first_value_cot.astype(jnp.float32) - column_lambda[None, :] * second_value_cot.astype(jnp.float32)).astype(jnp.bfloat16)
    gate_grad = across_tokens(normed_input, gate_cotangent)
    value_grad = across_tokens(normed_input, value_cot)
    gate_parts = optimizer_step(gate_weight, gate_first, gate_second, gate_grad, projection)
    value_parts = optimizer_step(value_weight, value_first, value_second, value_grad, projection)
    return (gate_parts[0], gate_parts[1], gate_parts[2], gate_parts[3], gate_parts[4], value_parts[0], value_parts[1], value_parts[2], value_parts[3], value_parts[4])
```

```python
import functools

import jax
import jax.numpy as jnp
from jax import lax
from jax.experimental import pallas as pl
from jax.experimental.pallas import tpu as pltpu
from jax.sharding import Mesh
from jax.sharding import PartitionSpec as P

D = 2048
RANK = 256
GATE = 256
VALUE = 128
BOTH = GATE + VALUE
NZ, NX, NY, NC = 8, 4, 4, 2
FS = ("z", "x")
TP = ("y", "c")
AXES = ("z", "x", "y", "c")
OWN = RANK // (NZ * NX)
ROWS = D // (NZ * NX)
TOKENS = 2048
CHUNKS = 4
CHUNK = TOKENS // CHUNKS

moment_decay = 0.9
square_decay = 0.95
adam_floor = 1e-08
learn_rate = 0.02
rms_floor = 0.1

MESH = pl.DeviceIdType.MESH
f32 = jnp.float32
bf16 = jnp.bfloat16


def moments(first, second, low):
    new_first = moment_decay * first + (1.0 - moment_decay) * low
    new_second = square_decay * second + (1.0 - square_decay) * low * low
    return new_first, new_second


def exchange_kernel(
    x_hbm, gate_hbm, one_hbm, two_hbm, lam_ref, proj_hbm, gw_hbm, vw_hbm, gf_hbm, gs_hbm, vf_hbm, vs_hbm,
    low_ref, upd_ref, wall_ref, tot_ref,
    xbuf, gbuf, onebuf, twobuf, pbuf, gwbuf, vwbuf, gfbuf, gsbuf, vfbuf, vsbuf,
    acc, part, landed, dirs,
    in_sems, x_sems, w_send, w_recv, rs_sems, ag_sems, tot_sems,
):
    z, x, y, c = [lax.axis_index(a) for a in AXES]
    me = z * NX + x
    my_tp = y * NC + c

    def at(dz, dx):
        return (lax.rem(z + dz, NZ), lax.rem(x + dx, NX), y, c)

    offsets = [(dz, dx) for dz in range(NZ) for dx in range(NX) if (dz, dx) != (0, 0)]
    tp_offsets = [(dy, dc) for dy in range(NY) for dc in range(NC) if (dy, dc) != (0, 0)]

    def tp_at(dy, dc):
        return (z, x, lax.rem(y + dy, NY), lax.rem(c + dc, NC))

    loads = [
        pltpu.make_async_copy(src, dst, in_sems.at[i])
        for i, (src, dst) in enumerate([
            (gw_hbm, gwbuf), (vw_hbm, vwbuf), (proj_hbm, pbuf), (gate_hbm, gbuf), (one_hbm, onebuf),
            (two_hbm, twobuf), (gf_hbm, gfbuf), (gs_hbm, gsbuf), (vf_hbm, vfbuf), (vs_hbm, vsbuf),
        ])
    ]
    x_loads = [
        pltpu.make_async_copy(
            x_hbm.at[pl.ds(i * CHUNK, CHUNK)], xbuf.at[pl.ds(i * CHUNK, CHUNK)], x_sems.at[i])
        for i in range(CHUNKS)
    ]
    for copy in loads[:3]:
        copy.start()
    x_loads[0].start()
    for copy in loads[3:6]:
        copy.start()
    for copy in x_loads[1:]:
        copy.start()
    for copy in loads[6:]:
        copy.start()

    barrier = pltpu.get_barrier_semaphore()
    for dz, dx in offsets:
        pl.semaphore_signal(barrier, inc=1, device_id=at(dz, dx), device_id_type=MESH)
    for dy, dc in tp_offsets:
        pl.semaphore_signal(barrier, inc=1, device_id=tp_at(dy, dc), device_id_type=MESH)

    loads[0].wait()
    loads[1].wait()
    wall_ref[x, z, :, 0:GATE] = gwbuf[...].astype(bf16)
    wall_ref[x, z, :, GATE:BOTH] = vwbuf[...].astype(bf16)
    loads[2].wait()

    pl.semaphore_wait(barrier, len(offsets) + len(tp_offsets))

    def remote(src, dst, send, recv, device):
        return pltpu.make_async_remote_copy(
            src_ref=src, dst_ref=dst, send_sem=send, recv_sem=recv, device_id=device, device_id_type=MESH)

    up, down = at(1, 0), at(NZ - 1, 0)
    east, west = at(0, 1), at(0, NX - 1)
    w_copies = []

    def w_step(step):
        pair = []
        for way, device in ((0, up), (1, down)):
            slot = lax.rem(z + (NZ - step if way == 0 else step), NZ)
            block = wall_ref.at[x, slot]
            if step == NZ // 2 - 1:
                block = block.at[pl.ds(way * (ROWS // 2), ROWS // 2)]
            pair.append(remote(block, block, w_send.at[2 * step + way], w_recv.at[2 * step + way], device))
        for copy in pair:
            copy.start()
        w_copies.append(pair)

    def w_landed(step):
        for copy in w_copies[step]:
            copy.wait_recv()

    w_step(0)

    def chunk(i):
        x_loads[i].wait()
        if i == 0:
            for copy in loads[3:6]:
                copy.wait()
        rows = pl.ds(i * CHUNK, CHUNK)
        projected = jnp.dot(xbuf[rows, :], pbuf[...], preferred_element_type=f32).astype(bf16)
        value_cot = (onebuf[rows, :].astype(f32) - lam_ref[0] * twobuf[rows, :].astype(f32)).astype(bf16)
        both = jnp.concatenate([gbuf[rows, :], value_cot], axis=1)
        term = lax.dot_general(projected, both, (((0,), (0,)), ((), ())), preferred_element_type=f32)
        if i == 0:
            acc[...] = term
        else:
            acc[...] += term

    chunk(0)
    w_landed(0)
    w_step(1)
    chunk(1)
    w_landed(1)
    w_step(2)
    chunk(2)
    w_landed(2)
    w_step(3)
    chunk(3)

    part[...] = acc[...].reshape(NZ * NX, OWN, BOTH).astype(bf16)
    rs_copies = []
    for j, (dz, dx) in enumerate(offsets):
        device = at(dz, dx)
        owner = device[0] * NX + device[1]
        rs_copies.append(remote(part.at[owner], landed.at[me], rs_sems.at[0, j], rs_sems.at[1, j], device))
        rs_copies[-1].start()
    for copy in loads[6:]:
        copy.wait()
    landed[me] = part[me]

    w_landed(3)
    column = wall_ref.at[x]
    x_copies = [
        remote(column, column, w_send.at[8], w_recv.at[8], east),
        remote(column, column, w_send.at[9], w_recv.at[9], west),
    ]

    for copy in rs_copies:
        copy.wait_recv()
    low = jnp.sum(landed[...].astype(f32), axis=0)
    low_ref[...] = low
    gate_first, gate_second = moments(gfbuf[...], gsbuf[...], low[:, 0:GATE])
    value_first, value_second = moments(vfbuf[...], vsbuf[...], low[:, GATE:BOTH])
    dirs[me, :, 0:GATE] = (gate_first / (jnp.sqrt(gate_second) + adam_floor)).astype(bf16)
    dirs[me, :, GATE:BOTH] = (value_first / (jnp.sqrt(value_second) + adam_floor)).astype(bf16)
    ag_copies = []
    for j, (dz, dx) in enumerate(offsets):
        ag_copies.append(remote(dirs.at[me], dirs.at[me], ag_sems.at[0, j], ag_sems.at[1, j], at(dz, dx)))
        ag_copies[-1].start()
    for copy in x_copies:
        copy.start()
    for copy in ag_copies:
        copy.wait_recv()

    spread = dirs[...].astype(f32).reshape(RANK, BOTH).astype(bf16)
    gate_sum = jnp.zeros((8, 128), f32)
    value_sum = jnp.zeros((8, 128), f32)
    for i in range(4):
        rows = pl.ds(i * 512, 512)
        update = jnp.dot(pbuf[rows, :], spread, preferred_element_type=f32)
        upd_ref[rows, :] = update
        squares = (update * update).reshape(64, 8, BOTH).sum(axis=0)
        gate_sum += squares[:, 0:128] + squares[:, 128:256]
        value_sum += squares[:, 256:384]
    tot_ref[my_tp, :, 0:128] = gate_sum
    tot_ref[my_tp, :, 128:256] = value_sum
    tot_copies = []
    for j, (dy, dc) in enumerate(tp_offsets):
        tot_copies.append(
            remote(tot_ref.at[my_tp], tot_ref.at[my_tp], tot_sems.at[0, j], tot_sems.at[1, j], tp_at(dy, dc)))
        tot_copies[-1].start()

    for copy in x_copies:
        copy.wait_recv()
    half = NZ // 2
    from_west = wall_ref.at[lax.rem(x + NX - 1, NX), pl.ds(0, half)]
    from_east = wall_ref.at[lax.rem(x + 1, NX), pl.ds(half, half)]
    far_copies = [
        remote(from_west, from_west, w_send.at[10], w_recv.at[10], east),
        remote(from_east, from_east, w_send.at[11], w_recv.at[11], west),
    ]
    for copy in far_copies:
        copy.start()
    for copy in tot_copies:
        copy.wait_recv()
    for copy in far_copies:
        copy.wait_recv()
    for pair in w_copies:
        for copy in pair:
            copy.wait_send()
    for copy in rs_copies + ag_copies + x_copies + far_copies + tot_copies:
        copy.wait_send()


def finish_kernel(
    low_ref, upd_ref, wall_ref, tot_ref, gw_ref, vw_ref, gf_ref, gs_ref, vf_ref, vs_ref,
    ngw_ref, gstep_ref, gcopy_hbm, ngf_ref, ngs_ref, nvw_ref, vstep_ref, vcopy_hbm, nvf_ref, nvs_ref,
    gout, vout, sems,
):
    z, x = lax.axis_index("z"), lax.axis_index("x")
    first_row = (z * NX + x) * ROWS
    totals = jnp.sum(tot_ref[...], axis=(0, 1))
    gate_total = jnp.sum(totals[0:128])
    value_total = jnp.sum(totals[128:256])
    gate_scale = 1.0 / (jnp.sqrt(jnp.full((8, 128), gate_total, f32) / (D * D)) + rms_floor)
    value_scale = 1.0 / (jnp.sqrt(jnp.full((8, 128), value_total, f32) / (D * 8 * VALUE)) + rms_floor)
    gate_scale = jnp.max(gate_scale)
    value_scale = jnp.max(value_scale)
    copies = []
    for f in range(NZ * NX):
        rows = pl.ds(f * ROWS, ROWS)
        update = upd_ref[rows, :]
        old = wall_ref[f % NX, f // NX].astype(f32)
        gout[rows, :] = (old[:, 0:GATE] - learn_rate * (update[:, 0:GATE] * gate_scale)).astype(bf16)
        vout[rows, :] = (old[:, GATE:BOTH] - learn_rate * (update[:, GATE:BOTH] * value_scale)).astype(bf16)
        if f % 8 == 7:
            span = pl.ds((f - 7) * ROWS, 8 * ROWS)
            n = f // 8
            copies.append(pltpu.make_async_copy(gout.at[span], gcopy_hbm.at[span], sems.at[2 * n]))
            copies.append(pltpu.make_async_copy(vout.at[span], vcopy_hbm.at[span], sems.at[2 * n + 1]))
            copies[-2].start()
            copies[-1].start()
    mine = upd_ref[pl.ds(pl.multiple_of(first_row, ROWS), ROWS), :]
    gate_step = mine[:, 0:GATE] * gate_scale
    value_step = mine[:, GATE:BOTH] * value_scale
    gstep_ref[...] = gate_step
    vstep_ref[...] = value_step
    ngw_ref[...] = gw_ref[...] - learn_rate * gate_step
    nvw_ref[...] = vw_ref[...] - learn_rate * value_step
    ngf_ref[...], ngs_ref[...] = moments(gf_ref[...], gs_ref[...], low_ref[:, 0:GATE])
    nvf_ref[...], nvs_ref[...] = moments(vf_ref[...], vs_ref[...], low_ref[:, GATE:BOTH])
    for copy in copies:
        copy.wait()


def per_device(
    normed_input, gate_cotangent, first_value_cot, second_value_cot, head_lambda, projection,
    gate_weight, gate_first, gate_second, value_weight, value_first, value_second,
):
    hbm = pl.BlockSpec(memory_space=pltpu.HBM)
    vmem = pl.BlockSpec(memory_space=pltpu.VMEM)
    smem = pl.BlockSpec(memory_space=pltpu.SMEM)
    peers = NZ * NX - 1
    low, upd, wall, tot = pl.pallas_call(
        exchange_kernel,
        name="exchange",
        in_specs=[hbm, hbm, hbm, hbm, smem, hbm, hbm, hbm, hbm, hbm, hbm, hbm],
        out_specs=[vmem] * 4,
        out_shape=[
            jax.ShapeDtypeStruct((OWN, BOTH), f32),
            jax.ShapeDtypeStruct((D, BOTH), f32),
            jax.ShapeDtypeStruct((NX, NZ, ROWS, BOTH), bf16),
            jax.ShapeDtypeStruct((NY * NC, 8, 256), f32),
        ],
        scratch_shapes=[
            pltpu.VMEM((TOKENS, D), bf16),
            pltpu.VMEM((TOKENS, GATE), bf16),
            pltpu.VMEM((TOKENS, VALUE), bf16),
            pltpu.VMEM((TOKENS, VALUE), bf16),
            pltpu.VMEM((D, RANK), bf16),
            pltpu.VMEM((ROWS, GATE), f32),
            pltpu.VMEM((ROWS, VALUE), f32),
            pltpu.VMEM((OWN, GATE), f32),
            pltpu.VMEM((OWN, GATE), f32),
            pltpu.VMEM((OWN, VALUE), f32),
            pltpu.VMEM((OWN, VALUE), f32),
            pltpu.VMEM((RANK, BOTH), f32),
            pltpu.VMEM((NZ * NX, OWN, BOTH), bf16),
            pltpu.VMEM((NZ * NX, OWN, BOTH), bf16),
            pltpu.VMEM((NZ * NX, OWN, BOTH), bf16),
            pltpu.SemaphoreType.DMA((10,)),
            pltpu.SemaphoreType.DMA((CHUNKS,)),
            pltpu.SemaphoreType.DMA((12,)),
            pltpu.SemaphoreType.DMA((12,)),
            pltpu.SemaphoreType.DMA((2, peers)),
            pltpu.SemaphoreType.DMA((2, peers)),
            pltpu.SemaphoreType.DMA((2, NY * NC - 1)),
        ],
        compiler_params=pltpu.CompilerParams(
            collective_id=0, has_side_effects=True, vmem_limit_bytes=40 * 1024 * 1024),
    )(normed_input, gate_cotangent, first_value_cot, second_value_cot, head_lambda, projection,
      gate_weight, value_weight, gate_first, gate_second, value_first, value_second)
    shape = jax.ShapeDtypeStruct
    return pl.pallas_call(
        finish_kernel,
        name="finish",
        in_specs=[vmem] * 10,
        out_specs=[vmem, vmem, hbm, vmem, vmem, vmem, vmem, hbm, vmem, vmem],
        out_shape=[
            shape((ROWS, GATE), f32), shape((ROWS, GATE), f32), shape((D, GATE), bf16),
            shape((OWN, GATE), f32), shape((OWN, GATE), f32),
            shape((ROWS, VALUE), f32), shape((ROWS, VALUE), f32), shape((D, VALUE), bf16),
            shape((OWN, VALUE), f32), shape((OWN, VALUE), f32),
        ],
        scratch_shapes=[
            pltpu.VMEM((D, GATE), bf16), pltpu.VMEM((D, VALUE), bf16), pltpu.SemaphoreType.DMA((8,)),
        ],
        compiler_params=pltpu.CompilerParams(vmem_limit_bytes=24 * 1024 * 1024),
    )(low, upd, wall, tot, gate_weight, value_weight, gate_first, gate_second, value_first, value_second)


def solution(mesh):
    torus = Mesh(mesh.devices.reshape(NZ, NX, NY, NC), AXES)
    split = P(FS, TP)
    return jax.shard_map(
        per_device,
        mesh=torus,
        in_specs=(P(FS, None), split, split, split, P(TP), P(), split, split, split, split, split, split),
        out_specs=(split, split, P(None, TP), split, split, split, split, P(None, TP), split, split),
        check_vma=False,
    )
```

```python
import functools

import jax
import jax.numpy as jnp
from jax import lax
from jax.experimental import pallas as pl
from jax.experimental.pallas import tpu as pltpu
from jax.sharding import Mesh
from jax.sharding import PartitionSpec as P

D = 2048
RANK = 256
GATE = 256
VALUE = 128
BOTH = GATE + VALUE
NZ, NX, NY, NC = 8, 4, 4, 2
FS = ("z", "x")
TP = ("y", "c")
AXES = ("z", "x", "y", "c")
OWN = RANK // (NZ * NX)
ROWS = D // (NZ * NX)
TOKENS = 2048
CHUNKS = 4
CHUNK = TOKENS // CHUNKS

moment_decay = 0.9
square_decay = 0.95
adam_floor = 1e-08
learn_rate = 0.02
rms_floor = 0.1

MESH = pl.DeviceIdType.MESH
f32 = jnp.float32
bf16 = jnp.bfloat16


def moments(first, second, low):
    new_first = moment_decay * first + (1.0 - moment_decay) * low
    new_second = square_decay * second + (1.0 - square_decay) * low * low
    return new_first, new_second


def exchange_kernel(
    x_hbm, gate_hbm, one_hbm, two_hbm, lam_ref, proj_hbm, gw_hbm, vw_hbm, gf_hbm, gs_hbm, vf_hbm, vs_hbm,
    low_ref, upd_ref, wall_ref, tot_ref,
    xbuf, gbuf, onebuf, twobuf, pbuf, gwbuf, vwbuf, gfbuf, gsbuf, vfbuf, vsbuf,
    ptbuf, acc, part, landed, dirs,
    in_sems, x_sems, w_sems, rs_sems, ag_sems, tot_sems,
):
    z, x, y, c = [lax.axis_index(a) for a in AXES]
    me = z * NX + x
    my_tp = y * NC + c

    def at(dz, dx):
        return (lax.rem(z + dz, NZ), lax.rem(x + dx, NX), y, c)

    offsets = sorted(
        [(dz, dx) for dz in range(NZ) for dx in range(NX) if (dz, dx) != (0, 0)],
        key=lambda o: -(min(o[0], NZ - o[0]) + min(o[1], NX - o[1])))
    tp_offsets = [(dy, dc) for dy in range(NY) for dc in range(NC) if (dy, dc) != (0, 0)]

    def tp_at(dy, dc):
        return (z, x, lax.rem(y + dy, NY), lax.rem(c + dc, NC))

    loads = [
        pltpu.make_async_copy(src, dst, in_sems.at[i])
        for i, (src, dst) in enumerate([
            (gw_hbm, gwbuf), (vw_hbm, vwbuf), (proj_hbm, pbuf), (gate_hbm, gbuf), (one_hbm, onebuf),
            (two_hbm, twobuf), (gf_hbm, gfbuf), (gs_hbm, gsbuf), (vf_hbm, vfbuf), (vs_hbm, vsbuf),
        ])
    ]
    x_loads = [
        pltpu.make_async_copy(
            x_hbm.at[pl.ds(i * CHUNK, CHUNK)], xbuf.at[pl.ds(i * CHUNK, CHUNK)], x_sems.at[i])
        for i in range(CHUNKS)
    ]
    for copy in loads[:3]:
        copy.start()
    x_loads[0].start()
    for copy in loads[3:6]:
        copy.start()
    for copy in x_loads[1:]:
        copy.start()
    for copy in loads[6:]:
        copy.start()

    barrier = pltpu.get_barrier_semaphore()
    for dz, dx in offsets:
        pl.semaphore_signal(barrier, inc=1, device_id=at(dz, dx), device_id_type=MESH)
    for dy, dc in tp_offsets:
        pl.semaphore_signal(barrier, inc=1, device_id=tp_at(dy, dc), device_id_type=MESH)

    loads[0].wait()
    loads[1].wait()
    wall_ref[x, z, :, 0:GATE] = gwbuf[...].astype(bf16)
    wall_ref[x, z, :, GATE:BOTH] = vwbuf[...].astype(bf16)
    loads[2].wait()
    ptbuf[...] = pbuf[...].T

    def remote(src, dst, send, recv, device):
        return pltpu.make_async_remote_copy(
            src_ref=src, dst_ref=dst, send_sem=send, recv_sem=recv, device_id=device, device_id_type=MESH)

    w_sent = []

    def w_copy(part, device):
        n = len(w_sent)
        copy = remote(part, part, w_sems.at[0, n], w_sems.at[1, n], device)
        copy.start()
        w_sent.append(copy)
        return copy

    def block(dz, dx=0):
        return wall_ref.at[lax.rem(x + dx + NX, NX), lax.rem(z + dz + NZ, NZ)]

    low_half, high_half = pl.ds(0, ROWS // 2), pl.ds(ROWS // 2, ROWS // 2)

    def to(dz, dx=0):
        return at(dz % NZ, dx % NX)

    def landed_from(copies):
        for copy in copies:
            copy.wait_recv()

    def beside(steps):
        return [w_copy(block(dz), to(0, dx)) for dz in steps for dx in (1, -1)]

    def across(steps):
        return [w_copy(block(dz, -dx).at[half], to(0, dx)) for dz in steps for dx, half in ((1, low_half), (-1, high_half))]

    near, far = (1, -1, 2, -2), (3, -3, 4)

    w = {}

    def w_start():
        w["z1"] = [w_copy(block(0), to(dz)) for dz in near]
        w["x0"] = beside((0,))

    def w_middle():
        landed_from(w["z1"])
        w["z2"] = [
            w_copy(block(-2), to(1)), w_copy(block(2), to(-1)),
            w_copy(block(-2).at[low_half], to(2)), w_copy(block(2).at[high_half], to(-2)),
        ]
        w["x1"] = beside(near)
        landed_from(w["x0"])
        w["f0"] = across((0,))

    def w_late():
        landed_from(w["z2"])
        w["x2"] = beside(far)
        landed_from(w["x1"])
        w["f1"] = across(near)

    def w_last():
        landed_from(w["x2"])
        w["f2"] = across(far)

    def chunk(i):
        x_loads[i].wait()
        if i == 0:
            for copy in loads[3:6]:
                copy.wait()
        rows = pl.ds(i * CHUNK, CHUNK)
        projected = lax.dot_general(
            ptbuf[...], xbuf[rows, :], (((1,), (1,)), ((), ())), preferred_element_type=f32).astype(bf16)
        value_cot = (onebuf[rows, :].astype(f32) - lam_ref[0] * twobuf[rows, :].astype(f32)).astype(bf16)
        both = jnp.concatenate([gbuf[rows, :], value_cot], axis=1)
        term = jnp.dot(projected, both, preferred_element_type=f32)
        if i == 0:
            acc[...] = term
        else:
            acc[...] += term

    for i in range(CHUNKS - 1):
        chunk(i)
    pl.semaphore_wait(barrier, len(offsets) + len(tp_offsets))
    w_start()
    chunk(CHUNKS - 1)

    part[...] = acc[...].reshape(NZ * NX, OWN, BOTH).astype(bf16)
    rs_copies = []
    for j, (dz, dx) in enumerate(offsets):
        device = at(dz, dx)
        owner = device[0] * NX + device[1]
        rs_copies.append(remote(part.at[owner], landed.at[me], rs_sems.at[0, j], rs_sems.at[1, j], device))
        rs_copies[-1].start()
    for copy in loads[6:]:
        copy.wait()
    landed[me] = part[me]

    w_middle()
    for copy in rs_copies:
        copy.wait_recv()
    low = jnp.sum(landed[...].astype(f32), axis=0)
    low_ref[...] = low
    gate_first, gate_second = moments(gfbuf[...], gsbuf[...], low[:, 0:GATE])
    value_first, value_second = moments(vfbuf[...], vsbuf[...], low[:, GATE:BOTH])
    dirs[me, :, 0:GATE] = (gate_first / (jnp.sqrt(gate_second) + adam_floor)).astype(bf16)
    dirs[me, :, GATE:BOTH] = (value_first / (jnp.sqrt(value_second) + adam_floor)).astype(bf16)
    ag_copies = []
    for j, (dz, dx) in enumerate(offsets):
        ag_copies.append(remote(dirs.at[me], dirs.at[me], ag_sems.at[0, j], ag_sems.at[1, j], at(dz, dx)))
        ag_copies[-1].start()
    w_late()
    for copy in ag_copies:
        copy.wait_recv()

    spread = dirs[...].astype(f32).reshape(RANK, BOTH).astype(bf16)
    gate_sum = jnp.zeros((8, 128), f32)
    value_sum = jnp.zeros((8, 128), f32)
    for i in range(4):
        rows = pl.ds(i * 512, 512)
        update = jnp.dot(pbuf[rows, :], spread, preferred_element_type=f32)
        upd_ref[rows, :] = update
        squares = (update * update).reshape(64, 8, BOTH).sum(axis=0)
        gate_sum += squares[:, 0:128] + squares[:, 128:256]
        value_sum += squares[:, 256:384]
    tot_ref[my_tp, 0:4, :] = gate_sum[0:4] + gate_sum[4:8]
    tot_ref[my_tp, 4:8, :] = value_sum[0:4] + value_sum[4:8]
    tot_copies = []
    for j, (dy, dc) in enumerate(tp_offsets):
        tot_copies.append(
            remote(tot_ref.at[my_tp], tot_ref.at[my_tp], tot_sems.at[0, j], tot_sems.at[1, j], tp_at(dy, dc)))
        tot_copies[-1].start()

    w_last()
    for copy in tot_copies:
        copy.wait_recv()
    for name in ("f0", "f1", "f2"):
        landed_from(w[name])
    for copy in w_sent + rs_copies + ag_copies + tot_copies:
        copy.wait_send()


def finish_kernel(
    low_ref, upd_ref, wall_ref, tot_ref, gw_ref, vw_ref, gf_ref, gs_ref, vf_ref, vs_ref,
    ngw_ref, gstep_ref, gcopy_hbm, ngf_ref, ngs_ref, nvw_ref, vstep_ref, vcopy_hbm, nvf_ref, nvs_ref,
    gout, vout, sems,
):
    z, x = lax.axis_index("z"), lax.axis_index("x")
    first_row = (z * NX + x) * ROWS
    totals = jnp.sum(tot_ref[...], axis=0)
    gate_total = jnp.sum(totals[0:4])
    value_total = jnp.sum(totals[4:8])
    gate_scale = 1.0 / (jnp.sqrt(jnp.full((8, 128), gate_total, f32) / (D * D)) + rms_floor)
    value_scale = 1.0 / (jnp.sqrt(jnp.full((8, 128), value_total, f32) / (D * 8 * VALUE)) + rms_floor)
    gate_scale = jnp.max(gate_scale)
    value_scale = jnp.max(value_scale)
    copies = []
    for f in range(NZ * NX):
        rows = pl.ds(f * ROWS, ROWS)
        update = upd_ref[rows, :]
        old = wall_ref[f % NX, f // NX].astype(f32)
        gout[rows, :] = (old[:, 0:GATE] - learn_rate * (update[:, 0:GATE] * gate_scale)).astype(bf16)
        vout[rows, :] = (old[:, GATE:BOTH] - learn_rate * (update[:, GATE:BOTH] * value_scale)).astype(bf16)
        if f % 8 == 7:
            span = pl.ds((f - 7) * ROWS, 8 * ROWS)
            n = f // 8
            copies.append(pltpu.make_async_copy(gout.at[span], gcopy_hbm.at[span], sems.at[2 * n]))
            copies.append(pltpu.make_async_copy(vout.at[span], vcopy_hbm.at[span], sems.at[2 * n + 1]))
            copies[-2].start()
            copies[-1].start()
    mine = upd_ref[pl.ds(pl.multiple_of(first_row, ROWS), ROWS), :]
    gate_step = mine[:, 0:GATE] * gate_scale
    value_step = mine[:, GATE:BOTH] * value_scale
    gstep_ref[...] = gate_step
    vstep_ref[...] = value_step
    ngw_ref[...] = gw_ref[...] - learn_rate * gate_step
    nvw_ref[...] = vw_ref[...] - learn_rate * value_step
    ngf_ref[...], ngs_ref[...] = moments(gf_ref[...], gs_ref[...], low_ref[:, 0:GATE])
    nvf_ref[...], nvs_ref[...] = moments(vf_ref[...], vs_ref[...], low_ref[:, GATE:BOTH])
    for copy in copies:
        copy.wait()


def per_device(
    normed_input, gate_cotangent, first_value_cot, second_value_cot, head_lambda, projection,
    gate_weight, gate_first, gate_second, value_weight, value_first, value_second,
):
    hbm = pl.BlockSpec(memory_space=pltpu.HBM)
    vmem = pl.BlockSpec(memory_space=pltpu.VMEM)
    smem = pl.BlockSpec(memory_space=pltpu.SMEM)
    peers = NZ * NX - 1
    low, upd, wall, tot = pl.pallas_call(
        exchange_kernel,
        name="exchange",
        in_specs=[hbm, hbm, hbm, hbm, smem, hbm, hbm, hbm, hbm, hbm, hbm, hbm],
        out_specs=[vmem] * 4,
        out_shape=[
            jax.ShapeDtypeStruct((OWN, BOTH), f32),
            jax.ShapeDtypeStruct((D, BOTH), f32),
            jax.ShapeDtypeStruct((NX, NZ, ROWS, BOTH), bf16),
            jax.ShapeDtypeStruct((NY * NC, 8, 128), f32),
        ],
        scratch_shapes=[
            pltpu.VMEM((TOKENS, D), bf16),
            pltpu.VMEM((TOKENS, GATE), bf16),
            pltpu.VMEM((TOKENS, VALUE), bf16),
            pltpu.VMEM((TOKENS, VALUE), bf16),
            pltpu.VMEM((D, RANK), bf16),
            pltpu.VMEM((ROWS, GATE), f32),
            pltpu.VMEM((ROWS, VALUE), f32),
            pltpu.VMEM((OWN, GATE), f32),
            pltpu.VMEM((OWN, GATE), f32),
            pltpu.VMEM((OWN, VALUE), f32),
            pltpu.VMEM((OWN, VALUE), f32),
            pltpu.VMEM((RANK, D), bf16),
            pltpu.VMEM((RANK, BOTH), f32),
            pltpu.VMEM((NZ * NX, OWN, BOTH), bf16),
            pltpu.VMEM((NZ * NX, OWN, BOTH), bf16),
            pltpu.VMEM((NZ * NX, OWN, BOTH), bf16),
            pltpu.SemaphoreType.DMA((10,)),
            pltpu.SemaphoreType.DMA((CHUNKS,)),
            pltpu.SemaphoreType.DMA((2, 42)),
            pltpu.SemaphoreType.DMA((2, peers)),
            pltpu.SemaphoreType.DMA((2, peers)),
            pltpu.SemaphoreType.DMA((2, NY * NC - 1)),
        ],
        compiler_params=pltpu.CompilerParams(
            collective_id=0, has_side_effects=True, vmem_limit_bytes=40 * 1024 * 1024),
    )(*[pltpu.with_memory_space_constraint(a, pltpu.HBM) for a in (normed_input, gate_cotangent, first_value_cot, second_value_cot)],
      head_lambda,
      *[pltpu.with_memory_space_constraint(a, pltpu.HBM) for a in (
          projection, gate_weight, value_weight, gate_first, gate_second, value_first, value_second)])
    shape = jax.ShapeDtypeStruct
    return pl.pallas_call(
        finish_kernel,
        name="finish",
        in_specs=[vmem] * 10,
        out_specs=[vmem, vmem, hbm, vmem, vmem, vmem, vmem, hbm, vmem, vmem],
        out_shape=[
            shape((ROWS, GATE), f32), shape((ROWS, GATE), f32), shape((D, GATE), bf16),
            shape((OWN, GATE), f32), shape((OWN, GATE), f32),
            shape((ROWS, VALUE), f32), shape((ROWS, VALUE), f32), shape((D, VALUE), bf16),
            shape((OWN, VALUE), f32), shape((OWN, VALUE), f32),
        ],
        scratch_shapes=[
            pltpu.VMEM((D, GATE), bf16), pltpu.VMEM((D, VALUE), bf16), pltpu.SemaphoreType.DMA((8,)),
        ],
        compiler_params=pltpu.CompilerParams(vmem_limit_bytes=24 * 1024 * 1024),
    )(low, upd, wall, tot, gate_weight, value_weight, gate_first, gate_second, value_first, value_second)


def solution(mesh):
    torus = Mesh(mesh.devices.reshape(NZ, NX, NY, NC), AXES)
    split = P(FS, TP)
    return jax.shard_map(
        per_device,
        mesh=torus,
        in_specs=(P(FS, None), split, split, split, P(TP), P(), split, split, split, split, split, split),
        out_specs=(split, split, P(None, TP), split, split, split, split, P(None, TP), split, split),
        check_vma=False,
    )
```

```python
import functools

import jax
import jax.numpy as jnp
from jax import lax
from jax.experimental import pallas as pl
from jax.experimental.pallas import tpu as pltpu
from jax.sharding import Mesh
from jax.sharding import PartitionSpec as P

D = 2048
RANK = 256
GATE = 256
VALUE = 128
BOTH = GATE + VALUE
NZ, NX, NY, NC = 8, 4, 4, 2
FS = ("z", "x")
TP = ("y", "c")
AXES = ("z", "x", "y", "c")
OWN = RANK // (NZ * NX)
ROWS = D // (NZ * NX)
TOKENS = 2048
CHUNKS = 4
CHUNK = TOKENS // CHUNKS

moment_decay = 0.9
square_decay = 0.95
adam_floor = 1e-08
learn_rate = 0.02
rms_floor = 0.1

MESH = pl.DeviceIdType.MESH
f32 = jnp.float32
bf16 = jnp.bfloat16


def moments(first, second, low):
    new_first = moment_decay * first + (1.0 - moment_decay) * low
    new_second = square_decay * second + (1.0 - square_decay) * low * low
    return new_first, new_second


def exchange_kernel(
    x_hbm, gate_hbm, one_hbm, two_hbm, lam_ref, proj_hbm, gw_hbm, vw_hbm, gf_hbm, gs_hbm, vf_hbm, vs_hbm,
    low_ref, upd_ref, wall_ref, tot_ref,
    xbuf, gbuf, onebuf, twobuf, pbuf, gwbuf, vwbuf, gfbuf, gsbuf, vfbuf, vsbuf,
    ptbuf, acc, part, landed, dirs,
    in_sems, w_sems, rs_sems, ag_sems, tot_sems,
):
    z, x, y, c = [lax.axis_index(a) for a in AXES]
    me = z * NX + x
    my_tp = y * NC + c
    peers, tp_peers = NZ * NX - 1, NY * NC - 1

    def at(dz, dx):
        return (lax.rem(z + dz, NZ), lax.rem(x + dx, NX), y, c)

    offsets = sorted(
        [(dz, dx) for dz in range(NZ) for dx in range(NX) if (dz, dx) != (0, 0)],
        key=lambda o: -(min(o[0], NZ - o[0]) + min(o[1], NX - o[1])))
    tp_offsets = [(dy, dc) for dy in range(NY) for dc in range(NC) if (dy, dc) != (0, 0)]

    def tp_at(dy, dc):
        return (z, x, lax.rem(y + dy, NY), lax.rem(c + dc, NC))

    def load(src, dst, n):
        pltpu.make_async_copy(src, dst, in_sems.at[n]).start()

    def take(sem, amount):
        pltpu.make_async_copy(amount, amount, sem).wait()

    def load_x(i):
        rows = pl.ds(i * CHUNK, CHUNK)
        load(x_hbm.at[rows], xbuf.at[rows], 4 + i)

    load(proj_hbm, pbuf, 0)
    load(gw_hbm, gwbuf, 1)
    load(vw_hbm, vwbuf, 1)
    load_x(0)

    barrier = pltpu.get_barrier_semaphore()
    for dz, dx in offsets:
        pl.semaphore_signal(barrier, inc=1, device_id=at(dz, dx), device_id_type=MESH)
    for dy, dc in tp_offsets:
        pl.semaphore_signal(barrier, inc=1, device_id=tp_at(dy, dc), device_id_type=MESH)

    load_x(1)
    take(in_sems.at[1], acc.at[pl.ds(0, 64)])
    wall_ref[x, z, :, 0:GATE] = gwbuf[...].astype(bf16)
    wall_ref[x, z, :, GATE:BOTH] = vwbuf[...].astype(bf16)
    take(in_sems.at[0], pbuf)
    load(gate_hbm, gbuf, 2)
    load(one_hbm, onebuf, 2)
    load(two_hbm, twobuf, 2)
    load_x(2)
    ptbuf[...] = pbuf[...].T

    def remote(src, dst, send, recv, device):
        return pltpu.make_async_remote_copy(
            src_ref=src, dst_ref=dst, send_sem=send, recv_sem=recv, device_id=device, device_id_type=MESH)

    def w_copy(part, device, group):
        remote(part, part, w_sems.at[0, group], w_sems.at[1, group], device).start()

    def w_blocks(group, blocks, way):
        take(w_sems.at[way, group], wall_ref.at[0, pl.ds(0, blocks)])

    def block(dz, dx=0):
        return wall_ref.at[lax.rem(x + dx + NX, NX), lax.rem(z + dz + NZ, NZ)]

    low_half, high_half = pl.ds(0, ROWS // 2), pl.ds(ROWS // 2, ROWS // 2)

    def to(dz, dx=0):
        return at(dz % NZ, dx % NX)

    def beside(steps, group):
        for dz in steps:
            for dx in (1, -1):
                w_copy(block(dz), to(0, dx), group)

    def across(steps):
        for dz in steps:
            for dx, half in ((1, low_half), (-1, high_half)):
                w_copy(block(dz, -dx).at[half], to(0, dx), 5)

    near, far = (1, -1, 2, -2), (3, -3, 4)

    group_blocks = (4, 2, 3, 8, 6, 8)

    def w_start():
        for dz in near:
            w_copy(block(0), to(dz), 0)
        beside((0,), 1)

    def w_middle():
        w_blocks(0, 4, 1)
        w_copy(block(-2), to(1), 2)
        w_copy(block(2), to(-1), 2)
        w_copy(block(-2).at[low_half], to(2), 2)
        w_copy(block(2).at[high_half], to(-2), 2)
        beside(near, 3)
        w_blocks(1, 2, 1)
        across((0,))

    def w_late():
        w_blocks(2, 3, 1)
        beside(far, 4)
        w_blocks(3, 8, 1)
        across(near)

    def w_last():
        w_blocks(4, 6, 1)
        across(far)

    def second(i, projected):
        rows = pl.ds(i * CHUNK, CHUNK)
        value_cot = (onebuf[rows, :].astype(f32) - lam_ref[0] * twobuf[rows, :].astype(f32)).astype(bf16)
        both = jnp.concatenate([gbuf[rows, :], value_cot], axis=1)
        term = jnp.dot(projected, both, preferred_element_type=f32)
        if i == 0:
            acc[...] = term
        else:
            acc[...] += term

    def chunk(i):
        rows = pl.ds(i * CHUNK, CHUNK)
        take(in_sems.at[4 + i], xbuf.at[rows])
        if i == 0:
            load_x(3)
            load(gf_hbm, gfbuf, 3)
            load(gs_hbm, gsbuf, 3)
            load(vf_hbm, vfbuf, 3)
            load(vs_hbm, vsbuf, 3)
        if i == 1:
            take(in_sems.at[2], xbuf.at[pl.ds(0, 512)])
        if i > 0:
            second(i - 1, held[0])
        held[0] = lax.dot_general(
            ptbuf[...], xbuf[rows, :], (((1,), (1,)), ((), ())), preferred_element_type=f32).astype(bf16)

    held = [None]
    for i in range(CHUNKS - 1):
        chunk(i)
    pl.semaphore_wait(barrier, len(offsets) + len(tp_offsets))
    w_start()
    chunk(CHUNKS - 1)
    second(CHUNKS - 1, held[0])

    part[...] = acc[...].reshape(NZ * NX, OWN, BOTH).astype(bf16)
    for dz, dx in offsets:
        device = at(dz, dx)
        owner = device[0] * NX + device[1]
        remote(part.at[owner], landed.at[me], rs_sems.at[0], rs_sems.at[1], device).start()
    take(in_sems.at[3], acc.at[pl.ds(0, 16)])
    landed[me] = part[me]

    w_middle()
    take(rs_sems.at[1], landed.at[pl.ds(0, peers)])
    low = jnp.sum(landed[...].astype(f32), axis=0)
    low_ref[...] = low
    gate_first, gate_second = moments(gfbuf[...], gsbuf[...], low[:, 0:GATE])
    value_first, value_second = moments(vfbuf[...], vsbuf[...], low[:, GATE:BOTH])
    dirs[me, :, 0:GATE] = (gate_first / (jnp.sqrt(gate_second) + adam_floor)).astype(bf16)
    dirs[me, :, GATE:BOTH] = (value_first / (jnp.sqrt(value_second) + adam_floor)).astype(bf16)
    for dz, dx in offsets:
        remote(dirs.at[me], dirs.at[me], ag_sems.at[0], ag_sems.at[1], at(dz, dx)).start()
    w_late()
    take(ag_sems.at[1], dirs.at[pl.ds(0, peers)])

    spread = dirs[...].astype(f32).reshape(RANK, BOTH).astype(bf16)
    gate_sum = jnp.zeros((8, 128), f32)
    value_sum = jnp.zeros((8, 128), f32)
    for i in range(4):
        rows = pl.ds(i * 512, 512)
        update = jnp.dot(pbuf[rows, :], spread, preferred_element_type=f32)
        upd_ref[rows, :] = update
        squares = (update * update).reshape(64, 8, BOTH).sum(axis=0)
        gate_sum += squares[:, 0:128] + squares[:, 128:256]
        value_sum += squares[:, 256:384]
    tot_ref[my_tp, 0:4, :] = gate_sum[0:4] + gate_sum[4:8]
    tot_ref[my_tp, 4:8, :] = value_sum[0:4] + value_sum[4:8]
    for dy, dc in tp_offsets:
        remote(tot_ref.at[my_tp], tot_ref.at[my_tp], tot_sems.at[0], tot_sems.at[1], tp_at(dy, dc)).start()

    w_last()
    take(tot_sems.at[1], tot_ref.at[pl.ds(0, tp_peers)])
    w_blocks(5, 8, 1)
    for group, blocks in enumerate(group_blocks):
        w_blocks(group, blocks, 0)
    take(rs_sems.at[0], part.at[pl.ds(0, peers)])
    take(ag_sems.at[0], dirs.at[pl.ds(0, peers)])
    take(tot_sems.at[0], tot_ref.at[pl.ds(0, tp_peers)])


def finish_kernel(
    low_ref, upd_ref, wall_ref, tot_ref, gw_ref, vw_ref, gf_ref, gs_ref, vf_ref, vs_ref,
    ngw_hbm, gstep_hbm, gcopy_hbm, ngf_hbm, ngs_hbm, nvw_hbm, vstep_hbm, vcopy_hbm, nvf_hbm, nvs_hbm,
    ngw, gstep, gout, ngf, ngs, nvw, vstep, vout, nvf, nvs, sems,
):
    z, x = lax.axis_index("z"), lax.axis_index("x")
    first_row = (z * NX + x) * ROWS
    totals = jnp.sum(tot_ref[...], axis=0)
    gate_total = jnp.sum(totals[0:4], keepdims=True)
    value_total = jnp.sum(totals[4:8], keepdims=True)
    gate_scale = 1.0 / (jnp.sqrt(gate_total / (D * D)) + rms_floor)
    value_scale = 1.0 / (jnp.sqrt(value_total / (D * 8 * VALUE)) + rms_floor)
    mine = upd_ref[pl.ds(pl.multiple_of(first_row, ROWS), ROWS), :]
    gate_step = mine[:, 0:GATE] * gate_scale
    value_step = mine[:, GATE:BOTH] * value_scale
    gstep[...] = gate_step
    vstep[...] = value_step
    ngw[...] = gw_ref[...] - learn_rate * gate_step
    nvw[...] = vw_ref[...] - learn_rate * value_step
    ngf[...], ngs[...] = moments(gf_ref[...], gs_ref[...], low_ref[:, 0:GATE])
    nvf[...], nvs[...] = moments(vf_ref[...], vs_ref[...], low_ref[:, GATE:BOTH])
    for src, dst in (
        (ngw, ngw_hbm), (gstep, gstep_hbm), (nvw, nvw_hbm), (vstep, vstep_hbm),
        (ngf, ngf_hbm), (ngs, ngs_hbm), (nvf, nvf_hbm), (nvs, nvs_hbm),
    ):
        pltpu.make_async_copy(src, dst, sems.at[0]).start()
    for f in range(NZ * NX):
        rows = pl.ds(f * ROWS, ROWS)
        update = upd_ref[rows, :]
        old = wall_ref[f % NX, f // NX].astype(f32)
        gout[rows, :] = (old[:, 0:GATE] - learn_rate * (update[:, 0:GATE] * gate_scale)).astype(bf16)
        vout[rows, :] = (old[:, GATE:BOTH] - learn_rate * (update[:, GATE:BOTH] * value_scale)).astype(bf16)
        if f % 4 == 3:
            span = pl.ds((f - 3) * ROWS, 4 * ROWS)
            pltpu.make_async_copy(gout.at[span], gcopy_hbm.at[span], sems.at[1]).start()
            pltpu.make_async_copy(vout.at[span], vcopy_hbm.at[span], sems.at[2]).start()
    small = upd_ref.at[pl.ds(0, 144)]
    pltpu.make_async_copy(small, small, sems.at[0]).wait()
    pltpu.make_async_copy(gout, gout, sems.at[1]).wait()
    pltpu.make_async_copy(vout, vout, sems.at[2]).wait()


def per_device(
    normed_input, gate_cotangent, first_value_cot, second_value_cot, head_lambda, projection,
    gate_weight, gate_first, gate_second, value_weight, value_first, value_second,
):
    hbm = pl.BlockSpec(memory_space=pltpu.HBM)
    vmem = pl.BlockSpec(memory_space=pltpu.VMEM)
    smem = pl.BlockSpec(memory_space=pltpu.SMEM)
    low, upd, wall, tot = pl.pallas_call(
        exchange_kernel,
        name="exchange",
        in_specs=[hbm, hbm, hbm, hbm, smem, hbm, hbm, hbm, hbm, hbm, hbm, hbm],
        out_specs=[vmem] * 4,
        out_shape=[
            jax.ShapeDtypeStruct((OWN, BOTH), f32),
            jax.ShapeDtypeStruct((D, BOTH), f32),
            jax.ShapeDtypeStruct((NX, NZ, ROWS, BOTH), bf16),
            jax.ShapeDtypeStruct((NY * NC, 8, 128), f32),
        ],
        scratch_shapes=[
            pltpu.VMEM((TOKENS, D), bf16),
            pltpu.VMEM((TOKENS, GATE), bf16),
            pltpu.VMEM((TOKENS, VALUE), bf16),
            pltpu.VMEM((TOKENS, VALUE), bf16),
            pltpu.VMEM((D, RANK), bf16),
            pltpu.VMEM((ROWS, GATE), f32),
            pltpu.VMEM((ROWS, VALUE), f32),
            pltpu.VMEM((OWN, GATE), f32),
            pltpu.VMEM((OWN, GATE), f32),
            pltpu.VMEM((OWN, VALUE), f32),
            pltpu.VMEM((OWN, VALUE), f32),
            pltpu.VMEM((RANK, D), bf16),
            pltpu.VMEM((RANK, BOTH), f32),
            pltpu.VMEM((NZ * NX, OWN, BOTH), bf16),
            pltpu.VMEM((NZ * NX, OWN, BOTH), bf16),
            pltpu.VMEM((NZ * NX, OWN, BOTH), bf16),
            pltpu.SemaphoreType.DMA((4 + CHUNKS,)),
            pltpu.SemaphoreType.DMA((2, 6)),
            pltpu.SemaphoreType.DMA((2,)),
            pltpu.SemaphoreType.DMA((2,)),
            pltpu.SemaphoreType.DMA((2,)),
        ],
        compiler_params=pltpu.CompilerParams(
            collective_id=0, has_side_effects=True, vmem_limit_bytes=40 * 1024 * 1024),
    )(*[a if a is head_lambda else pltpu.with_memory_space_constraint(a, pltpu.HBM) for a in (
        normed_input, gate_cotangent, first_value_cot, second_value_cot, head_lambda, projection,
        gate_weight, value_weight, gate_first, gate_second, value_first, value_second)])
    shape = jax.ShapeDtypeStruct
    outs = (
        ((ROWS, GATE), f32), ((ROWS, GATE), f32), ((D, GATE), bf16), ((OWN, GATE), f32), ((OWN, GATE), f32),
        ((ROWS, VALUE), f32), ((ROWS, VALUE), f32), ((D, VALUE), bf16), ((OWN, VALUE), f32), ((OWN, VALUE), f32),
    )
    return pl.pallas_call(
        finish_kernel,
        name="finish",
        in_specs=[vmem] * 10,
        out_specs=[hbm] * 10,
        out_shape=[shape(*o) for o in outs],
        scratch_shapes=[pltpu.VMEM(*o) for o in outs] + [pltpu.SemaphoreType.DMA((3,))],
        compiler_params=pltpu.CompilerParams(vmem_limit_bytes=24 * 1024 * 1024),
    )(low, upd, wall, tot, gate_weight, value_weight, gate_first, gate_second, value_first, value_second)


def solution(mesh):
    torus = Mesh(mesh.devices.reshape(NZ, NX, NY, NC), AXES)
    split = P(FS, TP)
    return jax.shard_map(
        per_device,
        mesh=torus,
        in_specs=(P(FS, None), split, split, split, P(TP), P(), split, split, split, split, split, split),
        out_specs=(split, split, P(None, TP), split, split, split, split, P(None, TP), split, split),
        check_vma=False,
    )
```

```python
import functools

import jax
import jax.numpy as jnp
from jax import lax
from jax.experimental import pallas as pl
from jax.experimental.pallas import tpu as pltpu
from jax.sharding import Mesh
from jax.sharding import PartitionSpec as P

D = 2048
RANK = 256
GATE = 256
VALUE = 128
BOTH = GATE + VALUE
NZ, NX, NY, NC = 8, 4, 4, 2
FS = ("z", "x")
TP = ("y", "c")
AXES = ("z", "x", "y", "c")
OWN = RANK // (NZ * NX)
ROWS = D // (NZ * NX)
TOKENS = 2048
CHUNKS = 4
CHUNK = TOKENS // CHUNKS

moment_decay = 0.9
square_decay = 0.95
adam_floor = 1e-08
learn_rate = 0.02
rms_floor = 0.1

MESH = pl.DeviceIdType.MESH
f32 = jnp.float32
bf16 = jnp.bfloat16


def moments(first, second, low):
    new_first = moment_decay * first + (1.0 - moment_decay) * low
    new_second = square_decay * second + (1.0 - square_decay) * low * low
    return new_first, new_second


def exchange_kernel(
    x_hbm, gate_hbm, one_hbm, two_hbm, lam_ref, proj_hbm, gw_hbm, vw_hbm, gf_hbm, gs_hbm, vf_hbm, vs_hbm,
    low_ref, upd_ref, wall_ref, tot_ref,
    xbuf, gbuf, onebuf, twobuf, pbuf, gwbuf, vwbuf, gfbuf, gsbuf, vfbuf, vsbuf,
    ptbuf, acc, part, landed, dirs,
    in_sems, w_sems, rs_sems, ag_sems, tot_sems,
):
    z, x, y, c = [lax.axis_index(a) for a in AXES]
    me = z * NX + x
    my_tp = y * NC + c
    peers, tp_peers = NZ * NX - 1, NY * NC - 1

    def at(dz, dx):
        return (lax.rem(z + dz, NZ), lax.rem(x + dx, NX), y, c)

    offsets = sorted(
        [(dz, dx) for dz in range(NZ) for dx in range(NX) if (dz, dx) != (0, 0)],
        key=lambda o: -(min(o[0], NZ - o[0]) + min(o[1], NX - o[1])))
    tp_offsets = [(dy, dc) for dy in range(NY) for dc in range(NC) if (dy, dc) != (0, 0)]

    def tp_at(dy, dc):
        return (z, x, lax.rem(y + dy, NY), lax.rem(c + dc, NC))

    def load(src, dst, n):
        pltpu.make_async_copy(src, dst, in_sems.at[n]).start()

    def take(sem, amount):
        pltpu.make_async_copy(amount, amount, sem).wait()

    def load_x(i):
        rows = pl.ds(i * CHUNK, CHUNK)
        load(x_hbm.at[rows], xbuf.at[rows], 4 + i)

    load(proj_hbm, pbuf, 0)
    load(gw_hbm, gwbuf, 1)
    load(vw_hbm, vwbuf, 1)
    load_x(0)

    barrier = pltpu.get_barrier_semaphore()
    for dz, dx in offsets:
        pl.semaphore_signal(barrier, inc=1, device_id=at(dz, dx), device_id_type=MESH)
    for dy, dc in tp_offsets:
        pl.semaphore_signal(barrier, inc=1, device_id=tp_at(dy, dc), device_id_type=MESH)

    load_x(1)
    take(in_sems.at[1], acc.at[pl.ds(0, 64)])
    wall_ref[x, z, :, 0:GATE] = gwbuf[...].astype(bf16)
    wall_ref[x, z, :, GATE:BOTH] = vwbuf[...].astype(bf16)
    take(in_sems.at[0], pbuf)
    load(gate_hbm, gbuf, 2)
    load(one_hbm, onebuf, 2)
    load(two_hbm, twobuf, 2)
    load_x(2)
    ptbuf[...] = pbuf[...].T

    def remote(src, dst, send, recv, device):
        return pltpu.make_async_remote_copy(
            src_ref=src, dst_ref=dst, send_sem=send, recv_sem=recv, device_id=device, device_id_type=MESH)

    def w_copy(part, device, group):
        remote(part, part, w_sems.at[0, group], w_sems.at[1, group], device).start()

    def w_blocks(group, blocks, way):
        take(w_sems.at[way, group], wall_ref.at[0, pl.ds(0, blocks)])

    def block(dz, dx=0):
        return wall_ref.at[lax.rem(x + dx + NX, NX), lax.rem(z + dz + NZ, NZ)]

    low_half, high_half = pl.ds(0, ROWS // 2), pl.ds(ROWS // 2, ROWS // 2)

    def to(dz, dx=0):
        return at(dz % NZ, dx % NX)

    def beside(steps, group):
        for dz in steps:
            for dx in (1, -1):
                w_copy(block(dz), to(0, dx), group)

    def across(steps):
        for dz in steps:
            for dx, half in ((1, low_half), (-1, high_half)):
                w_copy(block(dz, -dx).at[half], to(0, dx), 5)

    near, far = (1, -1, 2, -2), (3, -3, 4)

    group_blocks = (4, 2, 3, 8, 6, 8)

    def w_start():
        for dz in near:
            w_copy(block(0), to(dz), 0)
        beside((0,), 1)

    def w_middle():
        w_blocks(1, 2, 1)
        across((0,))
        w_blocks(0, 4, 1)
        w_copy(block(-2), to(1), 2)
        w_copy(block(2), to(-1), 2)
        w_copy(block(-2).at[low_half], to(2), 2)
        w_copy(block(2).at[high_half], to(-2), 2)
        beside(near, 3)

    def w_late():
        w_blocks(2, 3, 1)
        beside(far, 4)
        w_blocks(3, 8, 1)
        across(near)

    def w_last():
        w_blocks(4, 6, 1)
        across(far)

    def second(i, projected):
        rows = pl.ds(i * CHUNK, CHUNK)
        value_cot = (onebuf[rows, :].astype(f32) - lam_ref[0] * twobuf[rows, :].astype(f32)).astype(bf16)
        both = jnp.concatenate([gbuf[rows, :], value_cot], axis=1)
        term = jnp.dot(projected, both, preferred_element_type=f32)
        if i == 0:
            acc[...] = term
        else:
            acc[...] += term

    def chunk(i):
        rows = pl.ds(i * CHUNK, CHUNK)
        take(in_sems.at[4 + i], xbuf.at[rows])
        if i == 0:
            load_x(3)
            load(gf_hbm, gfbuf, 3)
            load(gs_hbm, gsbuf, 3)
            load(vf_hbm, vfbuf, 3)
            load(vs_hbm, vsbuf, 3)
        if i == 1:
            take(in_sems.at[2], xbuf.at[pl.ds(0, 512)])
        if i > 0:
            second(i - 1, held[0])
        held[0] = lax.dot_general(
            ptbuf[...], xbuf[rows, :], (((1,), (1,)), ((), ())), preferred_element_type=f32).astype(bf16)

    held = [None]
    for i in range(CHUNKS):
        if i == 1:
            pl.semaphore_wait(barrier, len(offsets) + len(tp_offsets))
            w_start()
        chunk(i)
    second(CHUNKS - 1, held[0])

    part[...] = acc[...].reshape(NZ * NX, OWN, BOTH).astype(bf16)
    for dz, dx in offsets:
        device = at(dz, dx)
        owner = device[0] * NX + device[1]
        remote(part.at[owner], landed.at[me], rs_sems.at[0], rs_sems.at[1], device).start()
    take(in_sems.at[3], acc.at[pl.ds(0, 16)])
    landed[me] = part[me]

    w_middle()
    take(rs_sems.at[1], landed.at[pl.ds(0, peers)])
    low = jnp.sum(landed[...].astype(f32), axis=0)
    low_ref[...] = low
    gate_first, gate_second = moments(gfbuf[...], gsbuf[...], low[:, 0:GATE])
    value_first, value_second = moments(vfbuf[...], vsbuf[...], low[:, GATE:BOTH])
    dirs[me, :, 0:GATE] = (gate_first / (jnp.sqrt(gate_second) + adam_floor)).astype(bf16)
    dirs[me, :, GATE:BOTH] = (value_first / (jnp.sqrt(value_second) + adam_floor)).astype(bf16)
    for dz, dx in offsets:
        remote(dirs.at[me], dirs.at[me], ag_sems.at[0], ag_sems.at[1], at(dz, dx)).start()
    w_late()
    take(ag_sems.at[1], dirs.at[pl.ds(0, peers)])

    spread = dirs[...].astype(f32).reshape(RANK, BOTH).astype(bf16)
    gate_sum = jnp.zeros((8, 128), f32)
    value_sum = jnp.zeros((8, 128), f32)
    for i in range(4):
        rows = pl.ds(i * 512, 512)
        update = jnp.dot(pbuf[rows, :], spread, preferred_element_type=f32)
        upd_ref[rows, :] = update
        squares = (update * update).reshape(64, 8, BOTH).sum(axis=0)
        gate_sum += squares[:, 0:128] + squares[:, 128:256]
        value_sum += squares[:, 256:384]
    tot_ref[my_tp, 0:4, :] = gate_sum[0:4] + gate_sum[4:8]
    tot_ref[my_tp, 4:8, :] = value_sum[0:4] + value_sum[4:8]
    for dy, dc in tp_offsets:
        remote(tot_ref.at[my_tp], tot_ref.at[my_tp], tot_sems.at[0], tot_sems.at[1], tp_at(dy, dc)).start()

    w_last()
    take(tot_sems.at[1], tot_ref.at[pl.ds(0, tp_peers)])
    w_blocks(5, 8, 1)
    for group, blocks in enumerate(group_blocks):
        w_blocks(group, blocks, 0)
    take(rs_sems.at[0], part.at[pl.ds(0, peers)])
    take(ag_sems.at[0], dirs.at[pl.ds(0, peers)])
    take(tot_sems.at[0], tot_ref.at[pl.ds(0, tp_peers)])


def finish_kernel(
    low_ref, upd_ref, wall_ref, tot_ref, gw_ref, vw_ref, gf_ref, gs_ref, vf_ref, vs_ref,
    ngw_hbm, gstep_hbm, gcopy_hbm, ngf_hbm, ngs_hbm, nvw_hbm, vstep_hbm, vcopy_hbm, nvf_hbm, nvs_hbm,
    ngw, gstep, gout, ngf, ngs, nvw, vstep, vout, nvf, nvs, sems,
):
    z, x = lax.axis_index("z"), lax.axis_index("x")
    first_row = (z * NX + x) * ROWS
    totals = jnp.sum(tot_ref[...], axis=0)
    gate_total = jnp.sum(totals[0:4], keepdims=True)
    value_total = jnp.sum(totals[4:8], keepdims=True)
    gate_scale = 1.0 / (jnp.sqrt(gate_total / (D * D)) + rms_floor)
    value_scale = 1.0 / (jnp.sqrt(value_total / (D * 8 * VALUE)) + rms_floor)
    mine = upd_ref[pl.ds(pl.multiple_of(first_row, ROWS), ROWS), :]
    gate_step = mine[:, 0:GATE] * gate_scale
    value_step = mine[:, GATE:BOTH] * value_scale
    gstep[...] = gate_step
    vstep[...] = value_step
    ngw[...] = gw_ref[...] - learn_rate * gate_step
    nvw[...] = vw_ref[...] - learn_rate * value_step
    ngf[...], ngs[...] = moments(gf_ref[...], gs_ref[...], low_ref[:, 0:GATE])
    nvf[...], nvs[...] = moments(vf_ref[...], vs_ref[...], low_ref[:, GATE:BOTH])
    for src, dst in (
        (ngw, ngw_hbm), (gstep, gstep_hbm), (nvw, nvw_hbm), (vstep, vstep_hbm),
        (ngf, ngf_hbm), (ngs, ngs_hbm), (nvf, nvf_hbm), (nvs, nvs_hbm),
    ):
        pltpu.make_async_copy(src, dst, sems.at[0]).start()
    for f in range(NZ * NX):
        rows = pl.ds(f * ROWS, ROWS)
        update = upd_ref[rows, :]
        old = wall_ref[f % NX, f // NX].astype(f32)
        gout[rows, :] = (old[:, 0:GATE] - learn_rate * (update[:, 0:GATE] * gate_scale)).astype(bf16)
        vout[rows, :] = (old[:, GATE:BOTH] - learn_rate * (update[:, GATE:BOTH] * value_scale)).astype(bf16)
        if f % 4 == 3:
            span = pl.ds((f - 3) * ROWS, 4 * ROWS)
            pltpu.make_async_copy(gout.at[span], gcopy_hbm.at[span], sems.at[1]).start()
            pltpu.make_async_copy(vout.at[span], vcopy_hbm.at[span], sems.at[2]).start()
    small = upd_ref.at[pl.ds(0, 144)]
    pltpu.make_async_copy(small, small, sems.at[0]).wait()
    pltpu.make_async_copy(gout, gout, sems.at[1]).wait()
    pltpu.make_async_copy(vout, vout, sems.at[2]).wait()


def per_device(
    normed_input, gate_cotangent, first_value_cot, second_value_cot, head_lambda, projection,
    gate_weight, gate_first, gate_second, value_weight, value_first, value_second,
):
    hbm = pl.BlockSpec(memory_space=pltpu.HBM)
    vmem = pl.BlockSpec(memory_space=pltpu.VMEM)
    smem = pl.BlockSpec(memory_space=pltpu.SMEM)
    low, upd, wall, tot = pl.pallas_call(
        exchange_kernel,
        name="exchange",
        in_specs=[hbm, hbm, hbm, hbm, smem, hbm, hbm, hbm, hbm, hbm, hbm, hbm],
        out_specs=[vmem] * 4,
        out_shape=[
            jax.ShapeDtypeStruct((OWN, BOTH), f32),
            jax.ShapeDtypeStruct((D, BOTH), f32),
            jax.ShapeDtypeStruct((NX, NZ, ROWS, BOTH), bf16),
            jax.ShapeDtypeStruct((NY * NC, 8, 128), f32),
        ],
        scratch_shapes=[
            pltpu.VMEM((TOKENS, D), bf16),
            pltpu.VMEM((TOKENS, GATE), bf16),
            pltpu.VMEM((TOKENS, VALUE), bf16),
            pltpu.VMEM((TOKENS, VALUE), bf16),
            pltpu.VMEM((D, RANK), bf16),
            pltpu.VMEM((ROWS, GATE), f32),
            pltpu.VMEM((ROWS, VALUE), f32),
            pltpu.VMEM((OWN, GATE), f32),
            pltpu.VMEM((OWN, GATE), f32),
            pltpu.VMEM((OWN, VALUE), f32),
            pltpu.VMEM((OWN, VALUE), f32),
            pltpu.VMEM((RANK, D), bf16),
            pltpu.VMEM((RANK, BOTH), f32),
            pltpu.VMEM((NZ * NX, OWN, BOTH), bf16),
            pltpu.VMEM((NZ * NX, OWN, BOTH), bf16),
            pltpu.VMEM((NZ * NX, OWN, BOTH), bf16),
            pltpu.SemaphoreType.DMA((4 + CHUNKS,)),
            pltpu.SemaphoreType.DMA((2, 6)),
            pltpu.SemaphoreType.DMA((2,)),
            pltpu.SemaphoreType.DMA((2,)),
            pltpu.SemaphoreType.DMA((2,)),
        ],
        compiler_params=pltpu.CompilerParams(
            collective_id=0, has_side_effects=True, vmem_limit_bytes=40 * 1024 * 1024),
    )(*[a if a is head_lambda else pltpu.with_memory_space_constraint(a, pltpu.HBM) for a in (
        normed_input, gate_cotangent, first_value_cot, second_value_cot, head_lambda, projection,
        gate_weight, value_weight, gate_first, gate_second, value_first, value_second)])
    shape = jax.ShapeDtypeStruct
    outs = (
        ((ROWS, GATE), f32), ((ROWS, GATE), f32), ((D, GATE), bf16), ((OWN, GATE), f32), ((OWN, GATE), f32),
        ((ROWS, VALUE), f32), ((ROWS, VALUE), f32), ((D, VALUE), bf16), ((OWN, VALUE), f32), ((OWN, VALUE), f32),
    )
    return pl.pallas_call(
        finish_kernel,
        name="finish",
        in_specs=[vmem] * 10,
        out_specs=[hbm] * 10,
        out_shape=[shape(*o) for o in outs],
        scratch_shapes=[pltpu.VMEM(*o) for o in outs] + [pltpu.SemaphoreType.DMA((3,))],
        compiler_params=pltpu.CompilerParams(vmem_limit_bytes=24 * 1024 * 1024),
    )(low, upd, wall, tot, gate_weight, value_weight, gate_first, gate_second, value_first, value_second)


def solution(mesh):
    torus = Mesh(mesh.devices.reshape(NZ, NX, NY, NC), AXES)
    split = P(FS, TP)
    return jax.shard_map(
        per_device,
        mesh=torus,
        in_specs=(P(FS, None), split, split, split, P(TP), P(), split, split, split, split, split, split),
        out_specs=(split, split, P(None, TP), split, split, split, split, P(None, TP), split, split),
        check_vma=False,
    )
```

```python
import functools

import jax
import jax.numpy as jnp
from jax import lax
from jax.experimental import pallas as pl
from jax.experimental.pallas import tpu as pltpu
from jax.sharding import Mesh
from jax.sharding import PartitionSpec as P

D = 2048
RANK = 256
GATE = 256
VALUE = 128
BOTH = GATE + VALUE
NZ, NX, NY, NC = 8, 4, 4, 2
FS = ("z", "x")
TP = ("y", "c")
AXES = ("z", "x", "y", "c")
OWN = RANK // (NZ * NX)
ROWS = D // (NZ * NX)
TOKENS = 2048
CHUNKS = 4
CHUNK = TOKENS // CHUNKS

moment_decay = 0.9
square_decay = 0.95
adam_floor = 1e-08
learn_rate = 0.02
rms_floor = 0.1

MESH = pl.DeviceIdType.MESH
f32 = jnp.float32
bf16 = jnp.bfloat16


def moments(first, second, low):
    new_first = moment_decay * first + (1.0 - moment_decay) * low
    new_second = square_decay * second + (1.0 - square_decay) * low * low
    return new_first, new_second


def exchange_kernel(
    x_hbm, gate_hbm, one_hbm, two_hbm, lam_ref, proj_hbm, gw_hbm, vw_hbm, gf_hbm, gs_hbm, vf_hbm, vs_hbm,
    low_ref, upd_ref, wall_ref, tot_ref,
    xbuf, gbuf, onebuf, twobuf, pbuf, gwbuf, vwbuf, gfbuf, gsbuf, vfbuf, vsbuf,
    ptbuf, gram, acc, part, landed, dirs,
    in_sems, w_sems, rs_sems, ag_sems, tot_sems,
):
    z, x, y, c = [lax.axis_index(a) for a in AXES]
    me = z * NX + x
    my_tp = y * NC + c
    peers, tp_peers = NZ * NX - 1, NY * NC - 1

    def at(dz, dx):
        return (lax.rem(z + dz, NZ), lax.rem(x + dx, NX), y, c)

    offsets = sorted(
        [(dz, dx) for dz in range(NZ) for dx in range(NX) if (dz, dx) != (0, 0)],
        key=lambda o: -(min(o[0], NZ - o[0]) + min(o[1], NX - o[1])))
    tp_offsets = sorted(
        [(dy, dc) for dy in range(NY) for dc in range(NC) if (dy, dc) != (0, 0)],
        key=lambda o: -(2 * min(o[0], NY - o[0]) + o[1]))

    def tp_at(dy, dc):
        return (z, x, lax.rem(y + dy, NY), lax.rem(c + dc, NC))

    def load(src, dst, n):
        pltpu.make_async_copy(src, dst, in_sems.at[n]).start()

    def take(sem, amount):
        pltpu.make_async_copy(amount, amount, sem).wait()

    def load_x(i):
        rows = pl.ds(i * CHUNK, CHUNK)
        load(x_hbm.at[rows], xbuf.at[rows], 4 + i)

    load(proj_hbm, pbuf, 0)
    load(gw_hbm, gwbuf, 1)
    load(vw_hbm, vwbuf, 1)
    load_x(0)

    barrier = pltpu.get_barrier_semaphore()
    for dz, dx in offsets:
        pl.semaphore_signal(barrier, inc=1, device_id=at(dz, dx), device_id_type=MESH)
    for dy, dc in tp_offsets:
        pl.semaphore_signal(barrier, inc=1, device_id=tp_at(dy, dc), device_id_type=MESH)

    load_x(1)
    take(in_sems.at[1], acc.at[pl.ds(0, 64)])
    wall_ref[x, z, :, 0:GATE] = gwbuf[...].astype(bf16)
    wall_ref[x, z, :, GATE:BOTH] = vwbuf[...].astype(bf16)
    take(in_sems.at[0], pbuf)
    load(gate_hbm, gbuf, 2)
    load(one_hbm, onebuf, 2)
    load(two_hbm, twobuf, 2)
    load_x(2)
    ptbuf[...] = pbuf[...].T

    def remote(src, dst, send, recv, device):
        return pltpu.make_async_remote_copy(
            src_ref=src, dst_ref=dst, send_sem=send, recv_sem=recv, device_id=device, device_id_type=MESH)

    def w_copy(part, device, group):
        remote(part, part, w_sems.at[0, group], w_sems.at[1, group], device).start()

    def w_blocks(group, blocks, way):
        take(w_sems.at[way, group], wall_ref.at[0, pl.ds(0, blocks)])

    def block(dz, dx=0):
        return wall_ref.at[lax.rem(x + dx + NX, NX), lax.rem(z + dz + NZ, NZ)]

    low_half, high_half = pl.ds(0, ROWS // 2), pl.ds(ROWS // 2, ROWS // 2)

    def to(dz, dx=0):
        return at(dz % NZ, dx % NX)

    def beside(steps, group):
        for dz in steps:
            for dx in (1, -1):
                w_copy(block(dz), to(0, dx), group)

    def across(steps):
        for dz in steps:
            for dx, half in ((1, low_half), (-1, high_half)):
                w_copy(block(dz, -dx).at[half], to(0, dx), 5)

    near, far = (1, -1, 2, -2), (3, -3, 4)

    group_blocks = (4, 2, 3, 8, 6, 8)

    def w_start():
        for dz in near:
            w_copy(block(0), to(dz), 0)
        beside((0,), 1)

    def w_middle():
        w_blocks(1, 2, 1)
        across((0,))
        w_blocks(0, 4, 1)
        beside(near, 3)
        w_copy(block(-2), to(1), 2)
        w_copy(block(2), to(-1), 2)
        w_copy(block(-2).at[low_half], to(2), 2)
        w_copy(block(2).at[high_half], to(-2), 2)

    def w_late():
        w_blocks(2, 3, 1)
        beside(far, 4)
        w_blocks(3, 8, 1)
        across(near)

    def w_last():
        w_blocks(4, 6, 1)
        across(far)

    def second(i, projected):
        rows = pl.ds(i * CHUNK, CHUNK)
        value_cot = (onebuf[rows, :].astype(f32) - lam_ref[0] * twobuf[rows, :].astype(f32)).astype(bf16)
        both = jnp.concatenate([gbuf[rows, :], value_cot], axis=1)
        term = jnp.dot(projected, both, preferred_element_type=f32)
        if i == 0:
            acc[...] = term
        else:
            acc[...] += term

    def chunk(i):
        rows = pl.ds(i * CHUNK, CHUNK)
        take(in_sems.at[4 + i], xbuf.at[rows])
        if i == 0:
            load_x(3)
            load(gf_hbm, gfbuf, 3)
            load(gs_hbm, gsbuf, 3)
            load(vf_hbm, vfbuf, 3)
            load(vs_hbm, vsbuf, 3)
        if i == 1:
            take(in_sems.at[2], xbuf.at[pl.ds(0, 512)])
        if i > 0:
            second(i - 1, held[0])
        held[0] = lax.dot_general(
            ptbuf[...], xbuf[rows, :], (((1,), (1,)), ((), ())), preferred_element_type=f32).astype(bf16)

    held = [None]
    for i in range(CHUNKS):
        if i == 1:
            pl.semaphore_wait(barrier, len(offsets) + len(tp_offsets))
            w_start()
        chunk(i)
    second(CHUNKS - 1, held[0])

    part[...] = acc[...].reshape(NZ * NX, OWN, BOTH).astype(bf16)
    for dz, dx in offsets:
        device = at(dz, dx)
        owner = device[0] * NX + device[1]
        remote(part.at[owner], landed.at[me], rs_sems.at[0], rs_sems.at[1], device).start()
    take(in_sems.at[3], acc.at[pl.ds(0, 16)])
    landed[me] = part[me]

    w_middle()
    products = lax.dot_general(ptbuf[...], pbuf[...], (((1,), (0,)), ((), ())), preferred_element_type=f32)
    for term in range(3):
        rounded = products.astype(bf16)
        gram[pl.ds(term * RANK, RANK), :] = rounded
        products = products - rounded.astype(f32)
    take(rs_sems.at[1], landed.at[pl.ds(0, peers)])
    low = jnp.sum(landed[...].astype(f32), axis=0)
    low_ref[...] = low
    gate_first, gate_second = moments(gfbuf[...], gsbuf[...], low[:, 0:GATE])
    value_first, value_second = moments(vfbuf[...], vsbuf[...], low[:, GATE:BOTH])
    dirs[me, :, 0:GATE] = (gate_first / (jnp.sqrt(gate_second) + adam_floor)).astype(bf16)
    dirs[me, :, GATE:BOTH] = (value_first / (jnp.sqrt(value_second) + adam_floor)).astype(bf16)
    for dz, dx in offsets:
        remote(dirs.at[me], dirs.at[me], ag_sems.at[0], ag_sems.at[1], at(dz, dx)).start()
    w_late()
    take(ag_sems.at[1], dirs.at[pl.ds(0, peers)])

    wide = dirs[...].astype(f32).reshape(RANK, BOTH)
    spread = wide.astype(bf16)
    terms = jnp.dot(gram[...], spread, preferred_element_type=f32)
    terms = (terms[2 * RANK:] + terms[RANK:2 * RANK]) + terms[0:RANK]
    squares = (wide * terms).reshape(RANK // 8, 8, BOTH).sum(axis=0)
    gate_sum = squares[:, 0:128] + squares[:, 128:256]
    value_sum = squares[:, 256:384]
    tot_ref[my_tp, 0:4, :] = gate_sum[0:4] + gate_sum[4:8]
    tot_ref[my_tp, 4:8, :] = value_sum[0:4] + value_sum[4:8]
    for dy, dc in tp_offsets:
        remote(tot_ref.at[my_tp], tot_ref.at[my_tp], tot_sems.at[0], tot_sems.at[1], tp_at(dy, dc)).start()

    w_last()
    for i in range(4):
        rows = pl.ds(i * 512, 512)
        upd_ref[rows, :] = jnp.dot(pbuf[rows, :], spread, preferred_element_type=f32)
    take(tot_sems.at[1], tot_ref.at[pl.ds(0, tp_peers)])
    w_blocks(5, 8, 1)
    for group, blocks in enumerate(group_blocks):
        w_blocks(group, blocks, 0)
    take(rs_sems.at[0], part.at[pl.ds(0, peers)])
    take(ag_sems.at[0], dirs.at[pl.ds(0, peers)])
    take(tot_sems.at[0], tot_ref.at[pl.ds(0, tp_peers)])


def finish_kernel(
    low_ref, upd_ref, wall_ref, tot_ref, gw_ref, vw_ref, gf_ref, gs_ref, vf_ref, vs_ref,
    ngw_hbm, gstep_hbm, gcopy_hbm, ngf_hbm, ngs_hbm, nvw_hbm, vstep_hbm, vcopy_hbm, nvf_hbm, nvs_hbm,
    ngw, gstep, gout, ngf, ngs, nvw, vstep, vout, nvf, nvs, sems,
):
    z, x = lax.axis_index("z"), lax.axis_index("x")
    first_row = (z * NX + x) * ROWS
    totals = jnp.sum(tot_ref[...], axis=0)
    gate_total = jnp.maximum(jnp.sum(totals[0:4], keepdims=True), 0.0)
    value_total = jnp.maximum(jnp.sum(totals[4:8], keepdims=True), 0.0)
    gate_scale = 1.0 / (jnp.sqrt(gate_total / (D * D)) + rms_floor)
    value_scale = 1.0 / (jnp.sqrt(value_total / (D * 8 * VALUE)) + rms_floor)
    mine = upd_ref[pl.ds(pl.multiple_of(first_row, ROWS), ROWS), :]
    gate_step = mine[:, 0:GATE] * gate_scale
    value_step = mine[:, GATE:BOTH] * value_scale
    gstep[...] = gate_step
    vstep[...] = value_step
    ngw[...] = gw_ref[...] - learn_rate * gate_step
    nvw[...] = vw_ref[...] - learn_rate * value_step
    ngf[...], ngs[...] = moments(gf_ref[...], gs_ref[...], low_ref[:, 0:GATE])
    nvf[...], nvs[...] = moments(vf_ref[...], vs_ref[...], low_ref[:, GATE:BOTH])
    for src, dst in (
        (ngw, ngw_hbm), (gstep, gstep_hbm), (nvw, nvw_hbm), (vstep, vstep_hbm),
        (ngf, ngf_hbm), (ngs, ngs_hbm), (nvf, nvf_hbm), (nvs, nvs_hbm),
    ):
        pltpu.make_async_copy(src, dst, sems.at[0]).start()
    for f in range(NZ * NX):
        rows = pl.ds(f * ROWS, ROWS)
        update = upd_ref[rows, :]
        old = wall_ref[f % NX, f // NX].astype(f32)
        gout[rows, :] = (old[:, 0:GATE] - learn_rate * (update[:, 0:GATE] * gate_scale)).astype(bf16)
        vout[rows, :] = (old[:, GATE:BOTH] - learn_rate * (update[:, GATE:BOTH] * value_scale)).astype(bf16)
        if f % 4 == 3:
            span = pl.ds((f - 3) * ROWS, 4 * ROWS)
            pltpu.make_async_copy(gout.at[span], gcopy_hbm.at[span], sems.at[1]).start()
            pltpu.make_async_copy(vout.at[span], vcopy_hbm.at[span], sems.at[2]).start()
    small = upd_ref.at[pl.ds(0, 144)]
    pltpu.make_async_copy(small, small, sems.at[0]).wait()
    pltpu.make_async_copy(gout, gout, sems.at[1]).wait()
    pltpu.make_async_copy(vout, vout, sems.at[2]).wait()


def per_device(
    normed_input, gate_cotangent, first_value_cot, second_value_cot, head_lambda, projection,
    gate_weight, gate_first, gate_second, value_weight, value_first, value_second,
):
    hbm = pl.BlockSpec(memory_space=pltpu.HBM)
    vmem = pl.BlockSpec(memory_space=pltpu.VMEM)
    smem = pl.BlockSpec(memory_space=pltpu.SMEM)
    low, upd, wall, tot = pl.pallas_call(
        exchange_kernel,
        name="exchange",
        in_specs=[hbm, hbm, hbm, hbm, smem, hbm, hbm, hbm, hbm, hbm, hbm, hbm],
        out_specs=[vmem] * 4,
        out_shape=[
            jax.ShapeDtypeStruct((OWN, BOTH), f32),
            jax.ShapeDtypeStruct((D, BOTH), f32),
            jax.ShapeDtypeStruct((NX, NZ, ROWS, BOTH), bf16),
            jax.ShapeDtypeStruct((NY * NC, 8, 128), f32),
        ],
        scratch_shapes=[
            pltpu.VMEM((TOKENS, D), bf16),
            pltpu.VMEM((TOKENS, GATE), bf16),
            pltpu.VMEM((TOKENS, VALUE), bf16),
            pltpu.VMEM((TOKENS, VALUE), bf16),
            pltpu.VMEM((D, RANK), bf16),
            pltpu.VMEM((ROWS, GATE), f32),
            pltpu.VMEM((ROWS, VALUE), f32),
            pltpu.VMEM((OWN, GATE), f32),
            pltpu.VMEM((OWN, GATE), f32),
            pltpu.VMEM((OWN, VALUE), f32),
            pltpu.VMEM((OWN, VALUE), f32),
            pltpu.VMEM((RANK, D), bf16),
            pltpu.VMEM((3 * RANK, RANK), bf16),
            pltpu.VMEM((RANK, BOTH), f32),
            pltpu.VMEM((NZ * NX, OWN, BOTH), bf16),
            pltpu.VMEM((NZ * NX, OWN, BOTH), bf16),
            pltpu.VMEM((NZ * NX, OWN, BOTH), bf16),
            pltpu.SemaphoreType.DMA((4 + CHUNKS,)),
            pltpu.SemaphoreType.DMA((2, 6)),
            pltpu.SemaphoreType.DMA((2,)),
            pltpu.SemaphoreType.DMA((2,)),
            pltpu.SemaphoreType.DMA((2,)),
        ],
        compiler_params=pltpu.CompilerParams(
            collective_id=0, has_side_effects=True, vmem_limit_bytes=40 * 1024 * 1024),
    )(*[a if a is head_lambda else pltpu.with_memory_space_constraint(a, pltpu.HBM) for a in (
        normed_input, gate_cotangent, first_value_cot, second_value_cot, head_lambda, projection,
        gate_weight, value_weight, gate_first, gate_second, value_first, value_second)])
    shape = jax.ShapeDtypeStruct
    outs = (
        ((ROWS, GATE), f32), ((ROWS, GATE), f32), ((D, GATE), bf16), ((OWN, GATE), f32), ((OWN, GATE), f32),
        ((ROWS, VALUE), f32), ((ROWS, VALUE), f32), ((D, VALUE), bf16), ((OWN, VALUE), f32), ((OWN, VALUE), f32),
    )
    return pl.pallas_call(
        finish_kernel,
        name="finish",
        in_specs=[vmem] * 10,
        out_specs=[hbm] * 10,
        out_shape=[shape(*o) for o in outs],
        scratch_shapes=[pltpu.VMEM(*o) for o in outs] + [pltpu.SemaphoreType.DMA((3,))],
        compiler_params=pltpu.CompilerParams(vmem_limit_bytes=24 * 1024 * 1024),
    )(low, upd, wall, tot, gate_weight, value_weight, gate_first, gate_second, value_first, value_second)


def solution(mesh):
    torus = Mesh(mesh.devices.reshape(NZ, NX, NY, NC), AXES)
    split = P(FS, TP)
    return jax.shard_map(
        per_device,
        mesh=torus,
        in_specs=(P(FS, None), split, split, split, P(TP), P(), split, split, split, split, split, split),
        out_specs=(split, split, P(None, TP), split, split, split, split, P(None, TP), split, split),
        check_vma=False,
    )
```
